32 devices in a mesh: ep: 8 (over z, core), tp: 4 (over y, x).
Axes of the slice: x: 2, y: 2, z: 4, core: 2. Of those that a mesh axis runs over, the one named last changes fastest.
Arguments:
- tokens: bfloat16 [1024, 2048], P('ep', 'tp'), may hold values from -6 to 6
- routing: int32 [1024, 2], P('ep'), may hold values from 0 to 3, all different within a row; in each aligned block of 128 rows (0 to 127, 128 to 255, ...) at most 80 rows name the same one
- mixing: float32 [1024, 2], P('ep'), may hold values from 0.1 to 0.9
- gate_matrix: bfloat16 [8, 2048, 2048], P('ep', None, 'tp'), may hold values from -0.125 to 0.125
- up_matrix: bfloat16 [8, 2048, 2048], P('ep', None, 'tp'), may hold values from -0.125 to 0.125
- down_matrix: bfloat16 [8, 2048, 2048], P('ep', 'tp'), may hold values from -0.09375 to 0.09375
- upstream: bfloat16 [1024, 2048], P('ep', 'tp'), may hold values from -6 to 6
Outputs:
- token_gradient: bfloat16 [1024, 2048], P('ep', 'tp')
- mixing_gradient: float32 [1024, 2], P('ep')
- gate_gradient: bfloat16 [8, 2048, 2048], P('ep', None, 'tp')
- up_gradient: bfloat16 [8, 2048, 2048], P('ep', None, 'tp')
- down_gradient: bfloat16 [8, 2048, 2048], P('ep', 'tp')
- input_norms: float32 [8, 2, 2048], P('ep')
- down_norms: float32 [8, 2048], P('ep', 'tp')
The draws below stay inside these ranges and needn't reach their ends.
Inputs may be any that keep to these rules, and one draw needn't show every extreme that they name: `routing`: A token's 2 experts differ. In each aligned block of 128 rows (the rows of one index of ep) no expert is named by more than 80 rows, and in every draw some expert is named by exactly 80 rows of some block.
All inputs are finite; a program needn't handle non-finite values.
Results may differ from the reference program's by a relative error of at most 0.0064.
Values may be sent and summed in bfloat16 or wider, within the bound.
No kernel may reach another device: no remote copies, remote signals or barrier semaphores. Data moves between devices by JAX's collectives and lax.ppermute only.
A program may use at most 64 MiB of HBM per device.

```python
import math
from functools import partial
import jax
import jax.numpy as jnp
import numpy as np
from jax import lax

D = 2048
FF = 4096
TOP = 2
TOK_DEV = 128
EXPERTS = 4
SLABS = 8
FF_HALF = 2048
CAP = 80
TOKENS = 1024
N_EP = 8
N_TP = 4


def levels(rng, extent, pieces, least, high):
    loudness = 1.0
    for axis_at, blocks in pieces:
        steps = jax.random.uniform(jax.random.fold_in(jax.random.fold_in(rng, 6), axis_at), (blocks,), jnp.float32, least / len(pieces), high / len(pieces))
        loudness = loudness * jnp.repeat(jnp.exp(steps), extent[axis_at] // blocks).reshape((-1,) + (1,) * (len(extent) - 1 - axis_at))
    return loudness


def routed_block(own_key, own, number, rows, count, top, bound, lean):
    ranking = jax.random.permutation(own_key, count)
    packed, common = shares(count, rows * top, bound, lean, True), shares(count, rows * top, bound, lean, False)
    places = jnp.arange(count)

    def named(lengths, turn):
        used = int((lengths > 0).sum())
        fixed = max(1, used // 4)
        shifted = fixed + (places - fixed + turn * (used - fixed)) % max(1, count - fixed)
        return jnp.zeros((count,), jnp.int32).at[ranking[jnp.where(places < fixed, places, shifted)]].set(jnp.asarray(lengths, jnp.int32))

    lengths = jnp.where(number % 4 == 0, named(packed, number // 4), named(common, number - number // 4 - 1))
    mixed = jax.random.permutation(jax.random.fold_in(own, 3), count)
    source_of, receiver = mixed[0:count // 2 * 2:2], mixed[1:count // 2 * 2:2]
    slack = jnp.minimum(lengths[source_of] - 1, bound - lengths[receiver]) // 2
    slack = jnp.where((source_of == ranking[0]) | (receiver == ranking[0]) | (lengths[receiver] == 0), 0, jnp.maximum(slack, 0))
    shifted = jax.random.randint(jax.random.fold_in(own, 4), (count // 2,), 0, 1 << 20) % (slack + 1)
    lengths = lengths.at[source_of].add(-shifted).at[receiver].add(shifted)
    members = jnp.searchsorted(jnp.cumsum(lengths), jnp.arange(rows * top), side="right").astype(jnp.int32)
    listing = members.reshape(top, rows).T
    listing = listing[jax.random.permutation(jax.random.fold_in(own, 1), rows)]
    turn = jax.random.randint(jax.random.fold_in(own, 2), (rows, 1), 0, top)
    return jnp.take_along_axis(listing, (jnp.arange(top)[None, :] + turn) % top, axis=1)


def shares(amount, total, most, skew, full):
    loads = [(1 << 20) // math.isqrt(rank ** skew) + 1 for rank in range(1, amount + 1)]
    largest = most if full else min(most, max(-(-total // amount), total * loads[0] // sum(loads)))
    least = 1 if total - largest >= amount - 1 else 0
    given, spare = [largest] + [least] * (amount - 1), total - largest - least * (amount - 1)
    while spare > 0:
        candidates = [i for i in range(1, amount) if given[i] < largest] or [i for i in range(1, amount) if given[i] < most]
        whole, budget = sum([loads[i] for i in candidates]), spare
        for i in candidates:
            addition = min(most - given[i], max(1, budget * loads[i] // whole), spare)
            given[i] = given[i] + addition
            spare = spare - addition
    return np.array(given)


def noise(own_key, extent, width, most, cuts=(), held_as=jnp.bfloat16):
    result = jax.random.normal(own_key, extent, jnp.float32) * width
    if len(cuts) > 0:
        result = levels(own_key, extent, cuts, -0.22, 0.18) * result
    return jnp.clip(result, min=-most, max=most).astype(held_as)


def setup_inputs(seed: int = 0) -> dict:
    key_list = jax.random.split(jax.random.key(seed), 8)
    tokens = noise(key_list[0], (TOKENS, D), 1.0, 6.0, ((0, 8), (1, 4)))
    routing_keys = jax.random.split(jax.random.fold_in(key_list[1], 1), TOKENS // TOK_DEV)
    routing_turns = jax.random.permutation(jax.random.fold_in(key_list[1], 3), TOKENS // TOK_DEV)
    routing = jax.vmap(lambda own, number: routed_block(jax.random.fold_in(key_list[1], 2), own, number, TOK_DEV, EXPERTS, TOP, CAP, 1))(routing_keys, routing_turns).reshape((TOKENS, TOP))
    mixing = jnp.clip(0.1 + 0.79999997 * jax.random.uniform(key_list[2], (TOKENS, TOP), jnp.float32) ** levels(key_list[2], (TOKENS, TOP), ((0, 8),), -0.2, 0.2), 0.1, 0.9)
    gate_matrix = noise(key_list[3], (SLABS, D, FF_HALF), D ** -0.5, 0.125, ((0, 8), (2, 4)))
    up_matrix = noise(key_list[4], (SLABS, D, FF_HALF), D ** -0.5, 0.125, ((0, 8), (2, 4)))
    down_matrix = noise(key_list[5], (SLABS, FF_HALF, D), FF ** -0.5, 0.09375, ((0, 8), (1, 4)))
    upstream = noise(key_list[6], (TOKENS, D), 1.0, 6.0, ((0, 8), (1, 4)))
    return dict(tokens=tokens, routing=routing, mixing=mixing, gate_matrix=gate_matrix, up_matrix=up_matrix, down_matrix=down_matrix, upstream=upstream)


def slot_targets(route_block, experts, capacity):
    flat_routes = route_block.reshape(-1).astype(jnp.int32)
    choose = (flat_routes[:, None] == jnp.arange(experts, dtype=jnp.int32)[None, :]).astype(jnp.int32)
    earlier = jnp.cumsum(choose, axis=0) - choose
    return (flat_routes * capacity + jnp.sum(earlier * choose, axis=1)).astype(jnp.int32)


def place_rows(target, values, slot_count):
    matches = (target[:, None] == jnp.arange(slot_count, dtype=jnp.int32)[None, :]).astype(values.dtype)
    placed = lax.dot_general(matches, values, (((0,), (0,)), ((), ())), preferred_element_type=jnp.float32)
    return placed.astype(jnp.bfloat16)


def take_rows(values, target):
    return jnp.take(values, target, axis=0)


def expert_backward(token_rows, grad_rows, gate_mat, up_mat, down_mat):
    gate_pre = jnp.dot(token_rows, gate_mat, preferred_element_type=jnp.float32)
    up_pre = jnp.dot(token_rows, up_mat, preferred_element_type=jnp.float32)
    sigmoid_gate = jax.nn.sigmoid(gate_pre)
    activated = gate_pre * sigmoid_gate
    hidden = activated * up_pre
    back_grad = lax.dot_general(grad_rows, down_mat, (((1,), (1,)), ((), ())), preferred_element_type=jnp.float32)
    up_grad = (back_grad * activated).astype(jnp.bfloat16)
    gate_grad = (back_grad * up_pre * sigmoid_gate * (1.0 + gate_pre * (1.0 - sigmoid_gate))).astype(jnp.bfloat16)
    hidden_low = hidden.astype(jnp.bfloat16)
    contract_rows = (((0,), (0,)), ((), ()))
    down_full = lax.dot_general(hidden_low, grad_rows, contract_rows, preferred_element_type=jnp.float32)
    gate_full = lax.dot_general(token_rows, gate_grad, contract_rows, preferred_element_type=jnp.float32)
    up_full = lax.dot_general(token_rows, up_grad, contract_rows, preferred_element_type=jnp.float32)
    scores = jnp.sum(hidden * back_grad, axis=1)
    return gate_full, up_full, down_full, gate_grad, up_grad, scores


def reference(tokens, routing, mixing, gate_matrix, up_matrix, down_matrix, upstream):
    sources = N_EP
    slot_count = EXPERTS * CAP
    route_blocks = routing.reshape(sources, TOK_DEV, TOP)
    targets = jax.vmap(partial(slot_targets, experts=EXPERTS, capacity=CAP))(route_blocks)
    scaled = (mixing[:, :, None] * upstream[:, None, :].astype(jnp.float32)).astype(jnp.bfloat16)
    spread_tokens = jnp.repeat(tokens.reshape(sources, TOK_DEV, D), TOP, axis=1)
    spread_grads = scaled.reshape(sources, TOK_DEV * TOP, D)
    placing = jax.vmap(partial(place_rows, slot_count=slot_count))

    def to_experts(placed):
        return placed.reshape(sources, EXPERTS, CAP, D).transpose(1, 0, 2, 3).reshape(EXPERTS, sources * CAP, D)

    expert_tokens = to_experts(placing(targets, spread_tokens))
    expert_grads = to_experts(placing(targets, spread_grads))
    gate_whole = gate_matrix.reshape(EXPERTS, 2, D, FF_HALF).transpose(0, 2, 1, 3).reshape(EXPERTS, D, FF)
    up_whole = up_matrix.reshape(EXPERTS, 2, D, FF_HALF).transpose(0, 2, 1, 3).reshape(EXPERTS, D, FF)
    down_whole = down_matrix.reshape(EXPERTS, FF, D)

    def one_expert(inputs):
        token_rows, grad_rows, gate_mat, up_mat, down_mat = inputs
        gate_full, up_full, down_full, gate_grad, up_grad, scores = expert_backward(token_rows, grad_rows, gate_mat, up_mat, down_mat)
        blocks = 2 * N_TP
        block_width = FF // blocks

        def add_block(block_index, running):
            start = (block_index * block_width).astype(jnp.int32)
            gate_piece = lax.dynamic_slice_in_dim(gate_grad, start, block_width, 1)
            up_piece = lax.dynamic_slice_in_dim(up_grad, start, block_width, 1)
            gate_cols = lax.dynamic_slice_in_dim(gate_mat, start, block_width, 1)
            up_cols = lax.dynamic_slice_in_dim(up_mat, start, block_width, 1)
            contract_cols = (((1,), (1,)), ((), ()))
            block_term = lax.dot_general(gate_piece, gate_cols, contract_cols, preferred_element_type=jnp.float32)
            block_term = block_term + lax.dot_general(up_piece, up_cols, contract_cols, preferred_element_type=jnp.float32)
            rounded = lax.optimization_barrier(block_term.astype(jnp.bfloat16))
            return running + rounded.astype(jnp.float32)

        pair_grad = lax.fori_loop(0, blocks, add_block, jnp.zeros((token_rows.shape[0], D), jnp.float32))
        gate_norm = jnp.sum(jnp.square(gate_full).reshape(D, 2, FF_HALF), axis=2).T
        up_norm = jnp.sum(jnp.square(up_full).reshape(D, 2, FF_HALF), axis=2).T
        input_norm = jnp.stack([gate_norm, up_norm], axis=1)
        down_norm = jnp.sum(down_full * down_full, axis=1)
        return (gate_full.astype(jnp.bfloat16), up_full.astype(jnp.bfloat16), down_full.astype(jnp.bfloat16),
                input_norm, down_norm, pair_grad, scores)

    results = lax.map(one_expert, (expert_tokens, expert_grads, gate_whole, up_whole, down_whole))
    gate_out, up_out, down_out, input_norm, down_norm, pair_grad, scores = results
    gate_gradient = gate_out.reshape(EXPERTS, D, 2, FF_HALF).transpose(0, 2, 1, 3).reshape(SLABS, D, FF_HALF)
    up_gradient = up_out.reshape(EXPERTS, D, 2, FF_HALF).transpose(0, 2, 1, 3).reshape(SLABS, D, FF_HALF)
    down_gradient = down_out.reshape(SLABS, FF_HALF, D)
    input_norms = input_norm.reshape(SLABS, 2, D)
    down_norms = down_norm.reshape(SLABS, FF_HALF)
    back_rows = pair_grad.reshape(EXPERTS, sources, CAP, D).transpose(1, 0, 2, 3).reshape(sources, slot_count, D)
    gathered_rows = jax.vmap(take_rows)(back_rows, targets)
    token_gradient = jnp.sum(gathered_rows.reshape(TOKENS, TOP, D), axis=1).astype(jnp.bfloat16)
    back_scores = scores.reshape(EXPERTS, sources, CAP).transpose(1, 0, 2).reshape(sources, slot_count)
    mixing_gradient = jax.vmap(take_rows)(back_scores, targets).reshape(TOKENS, TOP) / mixing
    return (token_gradient, mixing_gradient, gate_gradient, up_gradient, down_gradient, input_norms, down_norms)
```

```python
import functools

import jax
import jax.numpy as jnp
from jax import lax
from jax.experimental import pallas as pl
from jax.experimental.pallas import tpu as pltpu
from jax.sharding import PartitionSpec as P

F32 = jnp.float32
BF16 = jnp.bfloat16
VMEM = pl.BlockSpec(memory_space=pltpu.VMEM)
SMEM = pl.BlockSpec(memory_space=pltpu.SMEM)
MIB = 1 << 20


def dot(a, b, dims=((1,), (0,)), precision=None):
    return lax.dot_general(a, b, (dims, ((), ())), precision=precision, preferred_element_type=F32)


def call(body, outs, ins, mib, flops, name, grid=(), in_specs=None, out_specs=None, scratch=()):
    moved = sum(a.size * a.dtype.itemsize for a in (*ins, *outs))
    return pl.pallas_call(
        body,
        out_shape=outs,
        grid=grid,
        in_specs=in_specs,
        out_specs=out_specs or tuple(VMEM for _ in outs),
        scratch_shapes=scratch,
        compiler_params=pltpu.CompilerParams(vmem_limit_bytes=mib * MIB),
        cost_estimate=pl.CostEstimate(flops=flops, bytes_accessed=moved, transcendentals=0),
        name=name,
    )(*ins)


def out(shape, dtype=BF16):
    return jax.ShapeDtypeStruct(shape, dtype)


def place_body(experts, capacity, plane_ref, routing_ref, mixing_ref, tokens_ref, upstream_ref, target_ref, *pieces):
    rows, top = routing_ref.shape
    relative = routing_ref[...] - plane_ref[0]
    relative = jnp.where(relative < 0, relative + experts, relative)
    lanes = lax.broadcasted_iota(jnp.int32, (rows, 128), 1)
    chosen = [(relative[:, k : k + 1] == lanes).astype(F32) for k in range(top)]
    counts = functools.reduce(jnp.add, chosen).astype(BF16)
    before = (
        lax.broadcasted_iota(jnp.int32, (rows, rows), 0) > lax.broadcasted_iota(jnp.int32, (rows, rows), 1)
    ).astype(BF16)
    prior = dot(before, counts)
    slots = lax.broadcasted_iota(jnp.int32, (rows, experts * capacity), 1)
    upstream = upstream_ref[...].astype(F32)
    token_sum, grad_sum = None, None
    targets = []
    for k in range(top):
        slot = jnp.sum(prior * chosen[k], axis=1, keepdims=True).astype(jnp.int32)
        target = relative[:, k : k + 1] * capacity + slot
        targets.append(target)
        matches = (target == slots).astype(BF16)
        scaled = (mixing_ref[:, k : k + 1] * upstream).astype(BF16)
        token_part = dot(matches, tokens_ref[...], ((0,), (0,)))
        grad_part = dot(matches, scaled, ((0,), (0,)))
        token_sum = token_part if token_sum is None else token_sum + token_part
        grad_sum = grad_part if grad_sum is None else grad_sum + grad_part
    target_ref[...] = jnp.concatenate(targets, axis=1)
    for piece, piece_ref in enumerate(pieces):
        part = slice(piece * capacity, (piece + 1) * capacity)
        piece_ref[0] = token_sum[part].astype(BF16)
        piece_ref[1] = grad_sum[part].astype(BF16)


def hidden_body(
    place_ref, o0, o1, o2, o3t, o3g, p0, p1, p2, p3t, p3g, gate_ref, up_ref, down_ref,
    x_ref, y_ref, grads_ref, low_ref, score_ref, keep_ref, send_ref,
):
    place = place_ref[0]
    rows, width = o3t.shape
    count = gate_ref.shape[0] // width
    hidden_dev = gate_ref.shape[1]

    def columns(k):
        return pl.ds(pl.multiple_of((place ^ k) * width, width), width)

    for base, (b0, b1, b2, b3t, b3g) in ((0, (o0, o1, o2, o3t, o3g)), (rows, (p0, p1, p2, p3t, p3g))):
        for k, (x_part, y_part) in enumerate(
            ((b0[0], b0[1]), (b1[0], b1[1]), (b2[0], b2[1]), (b3t[...], b3g[...]))
        ):
            x_ref[base : base + rows, columns(k)] = x_part
            y_ref[base : base + rows, columns(k)] = y_part
    lane_sums = jnp.zeros((2 * rows, 128), F32)
    tile = 256
    for start in range(0, hidden_dev, tile):
        cols = slice(start, start + tile)
        gate_pre = dot(x_ref[...], gate_ref[:, cols])
        up_pre = dot(x_ref[...], up_ref[:, cols])
        back = dot(y_ref[...], down_ref[cols, :], ((1,), (1,)))
        sigmoid = jax.nn.sigmoid(gate_pre)
        activated = gate_pre * sigmoid
        hidden = activated * up_pre
        grads_ref[:, cols] = (back * up_pre * sigmoid * (1.0 + gate_pre * (1.0 - sigmoid))).astype(BF16)
        grads_ref[:, hidden_dev + start : hidden_dev + start + tile] = (back * activated).astype(BF16)
        low_ref[:, cols] = hidden.astype(BF16)
        score = hidden * back
        for lane in range(0, tile, 128):
            lane_sums += score[:, lane : lane + 128]
    score_ref[...] = dot(jnp.ones((8, 128), F32), lane_sums, ((1,), (1,)), lax.Precision.HIGHEST)
    for k in range(count):
        part = dot(grads_ref[:, :hidden_dev], gate_ref[columns(k), :], ((1,), (1,)))
        part += dot(grads_ref[:, hidden_dev:], up_ref[columns(k), :], ((1,), (1,)))
        keep_ref[k] = part[:rows]
        send_ref[k] = part[rows:].astype(BF16)


def weight_body(pieces, *refs):
    xs, ys = refs[:pieces], refs[pieces : 2 * pieces]
    grads, lows = refs[2 * pieces : 3 * pieces], refs[3 * pieces : 4 * pieces]
    gate_ref, up_ref, down_ref, norm_ref, down_norm_ref, sums_ref = refs[4 * pieces :]
    hidden_dev = gate_ref.shape[2]
    step = pl.program_id(0)

    def joined(parts):
        return jnp.concatenate([part[...] for part in parts], axis=0)

    def lane_sum(values):
        squares = values * values
        return functools.reduce(
            jnp.add, [squares[:, lane : lane + 128] for lane in range(0, values.shape[1], 128)]
        )

    def row_sum(sums):
        return dot(jnp.ones((8, 128), F32), sums, ((1,), (1,)), lax.Precision.HIGHEST)[0:1]

    x, y = joined(xs), joined(ys)
    grad, low = joined(grads), joined(lows)
    gate = dot(x, grad[:, :hidden_dev], ((0,), (0,)))
    gate_ref[0] = gate.astype(BF16)
    norm_ref[0:1, :] = row_sum(lane_sum(gate))
    up = dot(x, grad[:, hidden_dev:], ((0,), (0,)))
    up_ref[0] = up.astype(BF16)
    norm_ref[1:2, :] = row_sum(lane_sum(up))
    down = dot(low, y, ((0,), (0,)))
    down_ref[0] = down.astype(BF16)
    sums = lane_sum(down)

    @pl.when(step == 0)
    def _():
        sums_ref[...] = sums

    @pl.when(step > 0)
    def _():
        sums_ref[...] += sums

    @pl.when(step == pl.num_programs(0) - 1)
    def _():
        down_norm_ref[...] = row_sum(sums_ref[...])


def weight_grads(x, y, grads, low, full_width, hidden_dev):
    pieces = len(x)
    rows = x[0].shape[0]
    tile = 256
    whole = lambda width: [pl.BlockSpec((rows, width), lambda i: (0, 0))] * pieces
    tiled = [pl.BlockSpec((rows, tile), lambda i: (0, i))] * pieces
    return call(
        functools.partial(weight_body, pieces),
        (
            out((1, full_width, hidden_dev)),
            out((1, full_width, hidden_dev)),
            out((1, hidden_dev, full_width)),
            out((2, full_width), F32),
            out((1, hidden_dev), F32),
        ),
        (*x, *y, *grads, *low),
        40,
        6 * pieces * rows * full_width * hidden_dev,
        "weight_grads",
        grid=(full_width // tile,),
        in_specs=[*tiled, *tiled, *whole(2 * hidden_dev), *whole(hidden_dev)],
        out_specs=(
            pl.BlockSpec((1, tile, hidden_dev), lambda i: (0, i, 0)),
            pl.BlockSpec((1, tile, hidden_dev), lambda i: (0, i, 0)),
            pl.BlockSpec((1, hidden_dev, tile), lambda i: (0, 0, i)),
            pl.BlockSpec((2, tile), lambda i: (0, i)),
            pl.BlockSpec((1, hidden_dev), lambda i: (0, 0)),
        ),
        scratch=[pltpu.VMEM((hidden_dev, 128), F32)],
    )


def merge_body(keep_ref, came_ref, own_ref, x_ref, y_ref, d_ref):
    for k, target in enumerate((own_ref, x_ref, y_ref, d_ref)):
        target[...] = (keep_ref[k] + came_ref[k].astype(F32)).astype(BF16)


def finish_body(capacity, target_ref, mixing_ref, *refs):
    pieces = (len(refs) - 2) // 2
    rows_refs, score_refs = refs[:pieces], refs[pieces : 2 * pieces]
    token_ref, mix_ref = refs[2 * pieces :]
    rows, top = target_ref.shape
    lanes = lax.broadcasted_iota(jnp.int32, (rows, capacity), 1)
    total = None
    picked = [None] * top
    for piece in range(pieces):
        both = None
        for k in range(top):
            hit = target_ref[:, k : k + 1] == lanes + piece * capacity
            score = jnp.sum(jnp.where(hit, score_refs[piece][0:1, :], 0.0), axis=1, keepdims=True)
            picked[k] = score if picked[k] is None else picked[k] + score
            both = hit if both is None else both | hit
        part = dot(both.astype(BF16), rows_refs[piece][...])
        total = part if total is None else total + part
    token_ref[...] = total.astype(BF16)
    mix_ref[...] = jnp.concatenate(picked, axis=1) / mixing_ref[...]


def send(block, axis, destination):
    return lax.ppermute(block, axis, [(i, destination(i)) for i in range(lax.axis_size(axis))])


def fast(tokens, routing, mixing, gate_matrix, up_matrix, down_matrix, upstream):
    ep_count, tp_count = lax.axis_size("ep"), lax.axis_size("tp")
    planes = ep_count // 2
    tok_rows, width = tokens.shape
    top = routing.shape[1]
    capacity = 5 * top * tok_rows // (4 * planes)
    hidden_dev = gate_matrix.shape[2]
    full_width = tp_count * width
    plane = (lax.axis_index("ep") // 2).astype(jnp.int32).reshape(1)
    place = lax.axis_index("tp").astype(jnp.int32).reshape(1)

    def along(distance):
        return lambda i: (i // 2 + distance) % planes * 2 + i % 2

    swap, across_x, across_y = (lambda i: i ^ 1), (lambda i: i ^ 1), (lambda i: i ^ 2)
    target, *pieces = call(
        functools.partial(place_body, planes, capacity),
        (out((tok_rows, top), jnp.int32), *[out((2, capacity, width))] * planes),
        (plane, routing, mixing, tokens, upstream),
        16,
        4 * planes * capacity * tok_rows * top * width,
        "place",
        in_specs=[SMEM, VMEM, VMEM, VMEM, VMEM],
    )
    arrived = [pieces[0]] + [send(pieces[k], "ep", along(k)) for k in range(1, planes)]
    xs, ys, grads, lows, scores, sums = {}, {}, {}, {}, {}, {}
    order = [0, *sorted(range(1, planes), key=lambda k: min(k, planes - k))]
    for k in order:
        b0 = arrived[k]
        b1 = send(b0, "tp", across_x)
        b2 = send(b0, "tp", across_y)
        b3t = send(b1[0], "tp", across_y)
        b3g = send(b2[1], "tp", across_x)
        own = (b0, b1, b2, b3t, b3g)
        other = tuple(send(block, "ep", swap) for block in own)
        rows = 2 * capacity
        xs[k], ys[k], grads[k], lows[k], scores[k], keep, give = call(
            hidden_body,
            (
                out((rows, full_width)),
                out((rows, full_width)),
                out((rows, 2 * hidden_dev)),
                out((rows, hidden_dev)),
                out((8, rows), F32),
                out((tp_count, capacity, width), F32),
                out((tp_count, capacity, width)),
            ),
            (place, *own, *other, gate_matrix[0], up_matrix[0], down_matrix[0]),
            32,
            10 * rows * full_width * hidden_dev,
            "hidden",
            in_specs=[SMEM] + [VMEM] * 13,
        )
        came = send(give, "ep", swap)
        s0, s1, s2, s3 = call(
            merge_body, (out((capacity, width)),) * 4, (keep, came), 16, 1, "merge", in_specs=[VMEM] * 2
        )
        r1 = send(s1, "tp", across_x)
        r2 = send(s2, "tp", across_y)
        r3 = send(s3, "tp", lambda i: i ^ 3)
        sums[k] = (
            (s0.astype(F32) + r1.astype(F32)) + (r2.astype(F32) + r3.astype(F32))
        ).astype(BF16)
    back = [sums[0]] + [send(sums[k], "ep", along(-k)) for k in range(1, planes)]

    all_scores = jnp.stack([scores[k] for k in range(planes)])
    both = all_scores[:, :, :capacity] + send(all_scores[:, :, capacity:], "ep", swap)
    both = both + send(both, "tp", across_x)
    both = both + send(both, "tp", across_y)
    home = [both[0]] + [send(both[k], "ep", along(-k)) for k in range(1, planes)]

    ks = range(planes)
    gate, up, down, norms, down_norms = weight_grads(
        [xs[k] for k in ks], [ys[k] for k in ks], [grads[k] for k in ks], [lows[k] for k in ks],
        full_width, hidden_dev,
    )
    norms = norms + send(norms, "tp", across_x)
    norms = norms + send(norms, "tp", across_y)
    token_gradient, mixing_gradient = call(
        functools.partial(finish_body, capacity),
        (out((tok_rows, width)), out((tok_rows, top), F32)),
        (target, mixing, *back, *home),
        16,
        2 * tok_rows * planes * capacity * width,
        "finish",
        in_specs=[VMEM] * (2 + 2 * planes),
    )
    return token_gradient, mixing_gradient, gate, up, down, norms[None], down_norms


def swapped(block, axis, distance):
    count = lax.axis_size(axis)
    route = []
    for low in range(count):
        high = low | 1 << distance
        if high != low and high < count:
            route += [(low, high), (high, low)]
    return lax.ppermute(block, axis, route)


def slot_targets(route_block, experts, capacity):
    flat_routes = route_block.reshape(-1)
    choose = (flat_routes[:, None] == jnp.arange(experts, dtype=jnp.int32)[None, :]).astype(
        jnp.int32
    )
    earlier = jnp.cumsum(choose, axis=0) - choose
    return flat_routes * capacity + jnp.sum(earlier * choose, axis=1)


def place_rows(target, values, slot_count):
    matches = (target[:, None] == jnp.arange(slot_count, dtype=jnp.int32)[None, :]).astype(
        values.dtype
    )
    placed = lax.dot_general(
        matches, values, (((0,), (0,)), ((), ())), preferred_element_type=jnp.float32
    )
    return placed.astype(jnp.bfloat16)


def general(tokens, routing, mixing, gate_matrix, up_matrix, down_matrix, upstream):
    experts = lax.axis_size("ep") // 2
    tp_count = lax.axis_size("tp")
    tok_rows, part_width = tokens.shape
    top_count = routing.shape[1]
    capacity = 5 * top_count * tok_rows // (4 * experts)
    target = slot_targets(routing, experts, capacity)
    scaled = (mixing[:, :, None] * upstream[:, None, :].astype(jnp.float32)).astype(jnp.bfloat16)
    placed_tokens = place_rows(target, jnp.repeat(tokens, top_count, axis=0), experts * capacity)
    placed_grads = place_rows(
        target, scaled.reshape(tok_rows * top_count, part_width), experts * capacity
    )
    half_shape = (2 * experts, capacity // 2, part_width)
    arrived = (
        lax.all_to_all(
            placed_tokens.reshape(half_shape), "ep", split_axis=0, concat_axis=0, tiled=True
        ),
        lax.all_to_all(
            placed_grads.reshape(half_shape), "ep", split_axis=0, concat_axis=0, tiled=True
        ),
    )
    token_rows, grad_rows = (
        lax.all_gather(arrived[0][None], "tp", axis=0, tiled=True),
        lax.all_gather(arrived[1][None], "tp", axis=0, tiled=True),
    )
    other_tokens, other_grads = swapped((token_rows, grad_rows), "ep", 0)
    lower_half = lax.axis_index("ep") % 2 == 0
    token_rows = jnp.where(
        lower_half,
        jnp.concatenate([token_rows, other_tokens], axis=2),
        jnp.concatenate([other_tokens, token_rows], axis=2),
    )
    grad_rows = jnp.where(
        lower_half,
        jnp.concatenate([grad_rows, other_grads], axis=2),
        jnp.concatenate([other_grads, grad_rows], axis=2),
    )
    sources = token_rows.shape[1]
    row_count = sources * capacity
    token_blocks = token_rows.reshape(tp_count, row_count, part_width)
    grad_blocks = grad_rows.reshape(tp_count, row_count, part_width)
    hidden_dev = gate_matrix.shape[2]
    full_width = tp_count * part_width
    both_weights = jnp.concatenate([gate_matrix[0], up_matrix[0]], axis=1).reshape(
        tp_count, part_width, 2 * hidden_dev
    )
    down_blocks = down_matrix[0].reshape(hidden_dev, tp_count, part_width)
    both_pre = lax.dot_general(
        token_blocks, both_weights, (((0, 2), (0, 1)), ((), ())), preferred_element_type=jnp.float32
    )
    gate_pre = both_pre[:, :hidden_dev]
    up_pre = both_pre[:, hidden_dev:]
    sigmoid_gate = jax.nn.sigmoid(gate_pre)
    activated = gate_pre * sigmoid_gate
    hidden = activated * up_pre
    back_grad = lax.dot_general(
        grad_blocks, down_blocks, (((0, 2), (1, 2)), ((), ())), preferred_element_type=jnp.float32
    )
    gate_grad = (
        back_grad * up_pre * sigmoid_gate * (1.0 + gate_pre * (1.0 - sigmoid_gate))
    ).astype(jnp.bfloat16)
    up_grad = (back_grad * activated).astype(jnp.bfloat16)
    both_grad = jnp.concatenate([gate_grad, up_grad], axis=1)
    hidden_low = hidden.astype(jnp.bfloat16)
    down_full = lax.dot_general(
        hidden_low, grad_blocks, (((0,), (1,)), ((), ())), preferred_element_type=jnp.float32
    ).reshape(hidden_dev, full_width)
    both_full = lax.dot_general(
        token_blocks, both_grad, (((1,), (0,)), ((), ())), preferred_element_type=jnp.float32
    ).reshape(full_width, 2 * hidden_dev)
    gate_full = both_full[:, :hidden_dev]
    up_full = both_full[:, hidden_dev:]
    scores = jnp.sum(hidden * back_grad, axis=1)
    partial_rows = lax.dot_general(
        both_grad, both_weights, (((1,), (2,)), ((), ())), preferred_element_type=jnp.float32
    ).astype(jnp.bfloat16)
    pieces = lax.all_to_all(partial_rows, "tp", split_axis=1, concat_axis=1, tiled=True)
    summed = jnp.sum(pieces, axis=1, dtype=jnp.float32).reshape(sources, capacity, part_width)
    norm_terms = jnp.stack(
        [jnp.sum(gate_full * gate_full, axis=1), jnp.sum(up_full * up_full, axis=1)]
    )
    scores_all, norms_all = lax.psum((scores.reshape(sources, capacity), norm_terms), "tp")
    back_rows, back_scores = (
        lax.all_to_all(summed, "ep", split_axis=0, concat_axis=0, tiled=True),
        lax.all_to_all(scores_all, "ep", split_axis=0, concat_axis=0, tiled=True),
    )
    pair_rows = jnp.sum(back_rows.reshape(experts, 2, capacity, part_width), axis=1).reshape(
        experts * capacity, part_width
    )
    token_gradient = jnp.sum(
        jnp.take(pair_rows, target, axis=0).reshape(tok_rows, top_count, part_width), axis=1
    ).astype(jnp.bfloat16)
    pair_scores = jnp.sum(back_scores.reshape(experts, 2, capacity), axis=1).reshape(
        experts * capacity
    )
    mixing_gradient = jnp.take(pair_scores, target, axis=0).reshape(tok_rows, top_count) / mixing
    down_norms = jnp.sum(down_full * down_full, axis=1)
    return (
        token_gradient,
        mixing_gradient,
        gate_full.astype(jnp.bfloat16)[None],
        up_full.astype(jnp.bfloat16)[None],
        down_full.astype(jnp.bfloat16)[None],
        norms_all[None],
        down_norms[None],
    )


def solution(mesh):
    placed = (
        P("ep", "tp"),
        P("ep", None),
        P("ep", None),
        P("ep", None, "tp"),
        P("ep", None, "tp"),
        P("ep", "tp", None),
        P("ep", "tp"),
    )
    on_device = fast if mesh.shape["tp"] == 4 else general
    return jax.shard_map(
        on_device,
        mesh=mesh,
        in_specs=placed,
        out_specs=(
            P("ep", "tp"),
            P("ep", None),
            P("ep", None, "tp"),
            P("ep", None, "tp"),
            P("ep", "tp", None),
            P("ep", None, None),
            P("ep", "tp"),
        ),
        check_vma=False,
    )
```
